32 devices in a mesh: ep: 32 (over z, y, x, core).
Axes of the slice: x: 2, y: 2, z: 4, core: 2. Of those that a mesh axis runs over, the one named last changes fastest.
Arguments:
- hidden_in: bfloat16 [64, 2048], P('ep'), may hold values from -6 to 6
- lengths: int32 [64], P('ep'), may hold values from 1 to 1024, as said below
- key_cache: bfloat16 [64, 1024, 512], P('ep'), may hold values from -30 to 30
- value_cache: bfloat16 [64, 1024, 512], P('ep'), may hold values from -6 to 6
- query_w: bfloat16 [2048, 2048], P('ep'), may hold values from -0.125 to 0.125
- key_w: bfloat16 [2048, 512], P('ep'), may hold values from -0.125 to 0.125
- value_w: bfloat16 [2048, 512], P('ep'), may hold values from -0.125 to 0.125
- out_w: bfloat16 [2048, 2048], P('ep'), may hold values from -0.125 to 0.125
- lam_heads: float32 [8], replicated, may hold values from 0.3 to 0.8
- head_gain: float32 [256], replicated, may hold values from 0.1 to 1.9
- attn_gain: float32 [2048], replicated, may hold values from 0.1 to 1.9
- moe_gain: float32 [2048], replicated, may hold values from 0.1 to 1.9
- routing: int32 [64, 6], replicated, may hold values from 0 to 31, all different within a row; in each aligned block of 64 rows (0 to 63, 64 to 127, ...) at most 24 rows name the same one
- route_weight: float32 [64, 6], replicated, may hold values from 0.1 to 0.6
- gate_w: bfloat16 [32, 2048, 512], P('ep'), may hold values from -0.125 to 0.125
- up_w: bfloat16 [32, 2048, 512], P('ep'), may hold values from -0.125 to 0.125
- down_w: bfloat16 [32, 512, 2048], P('ep'), may hold values from -0.25 to 0.25
- shared_gate: bfloat16 [2048, 512], replicated, may hold values from -0.125 to 0.125
- shared_up: bfloat16 [2048, 512], replicated, may hold values from -0.125 to 0.125
- shared_down: bfloat16 [512, 2048], replicated, may hold values from -0.25 to 0.25
Outputs:
- layer_out: bfloat16 [64, 2048], P('ep')
- key_new: bfloat16 [64, 512], P('ep')
- value_new: bfloat16 [64, 512], P('ep')
The draws below stay inside these ranges and needn't reach their ends.
Inputs may be any that keep to these rules, and one draw needn't show every extreme that they name: `lengths`: some sequence has exactly 1024 positions in use. `routing`: each row names 6 different experts; no expert is named by more than 24 rows, a bound that some block reaches.
All inputs are finite; a program needn't handle non-finite values.
Results may differ from the reference program's by a relative error of at most 0.013.
The reference program's roundings to bfloat16 on the way count: a program that leaves them out, or rounds other values in their place, can miss the bound.
Values may be sent and summed in bfloat16 or wider, within the bound.
A program may use at most 64 MiB of HBM per device.

```python
import math
import jax
import jax.numpy as jnp
import numpy as np
from jax import lax

D = 2048
HEADS = 8
KV_HEADS = 2
HEAD_DIM = 128
VALUE_DIM = 256
EXPERT_DIM = 512
SHARED_DIM = 512
TOPK = 6
CACHE = 1024
SEQS = 64
EXPERTS = 32
EXP_CAP = 24


def draw_lengths(key, part):
    first_key, second_key = jax.random.split(key, 2)
    drawn = jax.random.randint(first_key, (SEQS,), 1, CACHE + 1, jnp.int32)
    chosen = jax.random.randint(second_key, (), 0, SEQS, jnp.int32)
    return jnp.where(jnp.arange(SEQS, dtype=jnp.int32) == chosen, CACHE, drawn).astype(jnp.int32)


def draw_key_cache(key, part):
    first_key = jax.random.fold_in(key, 0)
    shape = (SEQS, CACHE, KV_HEADS * 2 * HEAD_DIM)
    drawn = jnp.clip(1.75 * jax.random.normal(first_key, shape, jnp.float32), -14.0, 14.0)
    return drawn.astype(jnp.bfloat16)


def block_levels(own_key, extent, cuts, smallest, high):
    factor_of = 1.0
    for axis_at, shards_of in cuts:
        heights = jax.random.uniform(jax.random.fold_in(jax.random.fold_in(own_key, 6), axis_at), (shards_of,), jnp.float32, smallest / len(cuts), high / len(cuts))
        factor_of = factor_of * jnp.repeat(jnp.exp(heights), extent[axis_at] // shards_of).reshape((-1,) + (1,) * (len(extent) - 1 - axis_at))
    return factor_of


def deal_out(stream_key, own, number, rows, count, top, reach, slope):
    ranking = jax.random.permutation(stream_key, count)
    packed, ordinary = shares(count, rows * top, reach, slope, True), shares(count, rows * top, reach, slope, False)
    places = jnp.arange(count)

    def named(tallies, offset_by):
        used = int((tallies > 0).sum())
        fixed = max(1, used // 4)
        shifted = fixed + (places - fixed + offset_by * (used - fixed)) % max(1, count - fixed)
        return jnp.zeros((count,), jnp.int32).at[ranking[jnp.where(places < fixed, places, shifted)]].set(jnp.asarray(tallies, jnp.int32))

    tallies = jnp.where(number % 4 == 0, named(packed, number // 4), named(ordinary, number - number // 4 - 1))
    mixed = jax.random.permutation(jax.random.fold_in(own, 3), count)
    donor, receiver = mixed[0:count // 2 * 2:2], mixed[1:count // 2 * 2:2]
    margin = jnp.minimum(tallies[donor] - 1, reach - tallies[receiver]) // 2
    margin = jnp.where((donor == ranking[0]) | (receiver == ranking[0]) | (tallies[receiver] == 0), 0, jnp.maximum(margin, 0))
    shifted = jax.random.randint(jax.random.fold_in(own, 4), (count // 2,), 0, 1 << 20) % (margin + 1)
    tallies = tallies.at[donor].add(-shifted).at[receiver].add(shifted)
    items = jnp.searchsorted(jnp.cumsum(tallies), jnp.arange(rows * top), side="right").astype(jnp.int32)
    table = items.reshape(top, rows).T
    table = table[jax.random.permutation(jax.random.fold_in(own, 1), rows)]
    offset_by = jax.random.randint(jax.random.fold_in(own, 2), (rows, 1), 0, top)
    return jnp.take_along_axis(table, (jnp.arange(top)[None, :] + offset_by) % top, axis=1)


def shares(number_of, total, bound, lean, full):
    portions = [(1 << 20) // math.isqrt(grade ** lean) + 1 for grade in range(1, number_of + 1)]
    largest = bound if full else min(bound, max(-(-total // number_of), total * portions[0] // sum(portions)))
    least = 1 if total - largest >= number_of - 1 else 0
    counts, surplus = [largest] + [least] * (number_of - 1), total - largest - least * (number_of - 1)
    while surplus > 0:
        candidates = [i for i in range(1, number_of) if counts[i] < largest] or [i for i in range(1, number_of) if counts[i] < bound]
        whole, left = sum([portions[i] for i in candidates]), surplus
        for i in candidates:
            more = min(bound - counts[i], max(1, left * portions[i] // whole), surplus)
            counts[i] = counts[i] + more
            surplus = surplus - more
    return np.array(counts)


def noise(stream_key, shape, scale, most, pieces=(), kind=jnp.bfloat16):
    values = jax.random.normal(stream_key, shape, jnp.float32) * scale
    if len(pieces) > 0:
        values = block_levels(stream_key, shape, pieces, -0.22, 0.18) * values
    return jnp.clip(values, min=-most, max=most).astype(kind)


def setup_inputs(seed: int = 0) -> dict:
    key_list = jax.random.split(jax.random.key(seed), 21)
    hidden_in = noise(key_list[0], (SEQS, D), 1.0, 6.0, ((0, 32),))
    lengths = draw_lengths(jax.random.fold_in(key_list[20], 71), 0)
    key_cache = draw_key_cache(jax.random.fold_in(key_list[20], 71), 0)
    value_cache = noise(key_list[3], (SEQS, CACHE, KV_HEADS * VALUE_DIM), 1.0, 6.0, ((0, 32),))
    query_w = noise(key_list[4], (D, HEADS * 2 * HEAD_DIM), D ** -0.5, 0.125, ((0, 32),))
    key_w = noise(key_list[5], (D, KV_HEADS * 2 * HEAD_DIM), D ** -0.5, 0.125, ((0, 32),))
    value_w = noise(key_list[6], (D, KV_HEADS * VALUE_DIM), D ** -0.5, 0.125, ((0, 32),))
    out_w = noise(key_list[7], (HEADS * VALUE_DIM, D), (HEADS * VALUE_DIM) ** -0.5, 0.125, ((0, 32),))
    lam_heads = jnp.clip(jax.random.uniform(key_list[8], (HEADS,), jnp.float32, 0.3, 0.8), 0.3, 0.8)
    head_gain = jnp.clip(1.0 + 0.18 * jax.random.normal(key_list[9], (VALUE_DIM,), jnp.float32), 0.1, 1.9)
    attn_gain = jnp.clip(1.0 + 0.18 * jax.random.normal(key_list[10], (D,), jnp.float32), 0.1, 1.9)
    moe_gain = jnp.clip(1.0 + 0.18 * jax.random.normal(key_list[11], (D,), jnp.float32), 0.1, 1.9)
    routing_keys = jax.random.split(jax.random.fold_in(key_list[12], 1), SEQS // SEQS)
    routing_turns = jax.random.permutation(jax.random.fold_in(key_list[12], 3), SEQS // SEQS)
    routing = jax.vmap(lambda own, number: deal_out(jax.random.fold_in(key_list[12], 2), own, number, SEQS, EXPERTS, TOPK, EXP_CAP, 1))(routing_keys, routing_turns).reshape((SEQS, TOPK))
    route_weight = jnp.clip(jnp.exp(jax.random.uniform(key_list[13], (SEQS, TOPK), jnp.float32, math.log(0.1), math.log(0.6))), 0.1, 0.6)
    gate_w = noise(key_list[14], (EXPERTS, D, EXPERT_DIM), D ** -0.5, 0.125, ((0, 32),))
    up_w = noise(key_list[15], (EXPERTS, D, EXPERT_DIM), D ** -0.5, 0.125, ((0, 32),))
    down_w = noise(key_list[16], (EXPERTS, EXPERT_DIM, D), EXPERT_DIM ** -0.5, 0.25, ((0, 32),))
    shared_gate = noise(key_list[17], (D, SHARED_DIM), D ** -0.5, 0.125)
    shared_up = noise(key_list[18], (D, SHARED_DIM), D ** -0.5, 0.125)
    shared_down = noise(key_list[19], (SHARED_DIM, D), SHARED_DIM ** -0.5, 0.25)
    return dict(hidden_in=hidden_in, lengths=lengths, key_cache=key_cache, value_cache=value_cache, query_w=query_w, key_w=key_w, value_w=value_w, out_w=out_w, lam_heads=lam_heads, head_gain=head_gain, attn_gain=attn_gain, moe_gain=moe_gain, routing=routing, route_weight=route_weight, gate_w=gate_w, up_w=up_w, down_w=down_w, shared_gate=shared_gate, shared_up=shared_up, shared_down=shared_down)


eps_norm = 1e-06
eps_head = 1e-05
theta_base = 500000.0

def rms_scale(row_block, gain_vec, epsilon):
    row_block = row_block.astype(jnp.float32)
    return row_block * lax.rsqrt(lax.optimization_barrier(jnp.mean(row_block * row_block, axis=-1, keepdims=True)) + epsilon) * gain_vec.astype(jnp.float32)

def rotate(vectors, positions):
    half_width = vectors.shape[-1] // 2
    inverse = theta_base ** (-jnp.arange(half_width, dtype=jnp.float32) / half_width)
    angles = positions.astype(jnp.float32)[..., None] * inverse
    cosine, sine_part = (jnp.cos(angles), jnp.sin(angles))
    lower_half, upper_half = (vectors[..., :half_width], vectors[..., half_width:])
    return jnp.concatenate([lower_half * cosine - upper_half * sine_part, lower_half * sine_part + upper_half * cosine], axis=-1)

def attend(queries, key_new, value_new, cache_keys, cache_values, lengths, lam_heads, head_gain):
    num_seqs, kv_heads, group_size = (queries.shape[0], queries.shape[1], queries.shape[2])
    head_dim = queries.shape[-1]
    cache_len = cache_keys.shape[1]
    cache_keys = cache_keys.reshape(num_seqs, cache_len, kv_heads, 2, head_dim).astype(jnp.float32)
    cache_values = cache_values.reshape(num_seqs, cache_len, kv_heads, -1).astype(jnp.float32)
    value_new = value_new.reshape(num_seqs, kv_heads, -1)
    queries = queries.astype(jnp.float32)
    score_scale = head_dim ** (-0.5)
    scores = jnp.einsum('skgph,sckph->skgpc', queries, cache_keys) * score_scale
    self_score = jnp.einsum('skgph,skph->skgp', queries, key_new.astype(jnp.float32)) * score_scale
    live_mask = (jnp.arange(cache_len)[None, :] < lengths[:, None])[:, None, None, None, :]
    peak = jnp.maximum(lax.optimization_barrier(jnp.max(jnp.where(live_mask, scores, -jnp.inf), axis=-1)), self_score)
    weights = jnp.where(live_mask, jnp.exp(scores - peak[..., None]), 0.0)
    self_weight = jnp.exp(self_score - peak)
    totals = lax.optimization_barrier(jnp.sum(weights, axis=-1)) + self_weight
    lambda_grid = lam_heads.reshape(kv_heads, group_size)[None]
    combined = (weights[:, :, :, 0] / totals[:, :, :, 0, None] - lambda_grid[..., None] * weights[:, :, :, 1] / totals[:, :, :, 1, None]).astype(jnp.bfloat16)
    self_combined = (self_weight[..., 0] / totals[..., 0] - lambda_grid * self_weight[..., 1] / totals[..., 1]).astype(jnp.bfloat16)
    head_out = jnp.einsum('skgc,sckv->skgv', combined.astype(jnp.float32), cache_values)
    head_out = head_out + self_combined.astype(jnp.float32)[..., None] * value_new.astype(jnp.float32)[:, :, None, :]
    return rms_scale(head_out, head_gain, eps_head).astype(jnp.bfloat16).reshape(num_seqs, -1)

def routed_sum(moe_in, routing, route_weight, gate_w, up_w, down_w):

    def add_expert(running, expert_id):
        routed_here = lax.optimization_barrier(jnp.sum((routing == expert_id).astype(jnp.int32), axis=1))
        weight_col = lax.optimization_barrier(jnp.sum(jnp.where(routing == expert_id, route_weight, 0.0), axis=1))
        slot_index = jnp.cumsum(routed_here) - 1
        pick_table = ((slot_index[None, :] == jnp.arange(EXP_CAP)[:, None]) & (routed_here[None, :] > 0)).astype(jnp.float32)
        picked = jnp.dot(pick_table, moe_in.astype(jnp.float32)).astype(jnp.bfloat16)
        gate_one = lax.dynamic_index_in_dim(gate_w, expert_id, 0, keepdims=False)
        up_one = lax.dynamic_index_in_dim(up_w, expert_id, 0, keepdims=False)
        down_one = lax.dynamic_index_in_dim(down_w, expert_id, 0, keepdims=False)
        hidden = (jax.nn.silu(jnp.dot(picked, gate_one, preferred_element_type=jnp.float32)) * jnp.dot(picked, up_one, preferred_element_type=jnp.float32)).astype(jnp.bfloat16)
        result = jnp.dot(hidden, down_one, preferred_element_type=jnp.float32).astype(jnp.bfloat16)
        return (running + jnp.dot(pick_table.T, result.astype(jnp.float32)) * weight_col[:, None], None)
    start_sum = jnp.zeros(moe_in.shape, jnp.float32)
    running, unused = lax.scan(add_expert, start_sum, jnp.arange(gate_w.shape[0], dtype=jnp.int32))
    return running

def reference(hidden_in, lengths, key_cache, value_cache, query_w, key_w, value_w, out_w, lam_heads, head_gain, attn_gain, moe_gain, routing, route_weight, gate_w, up_w, down_w, shared_gate, shared_up, shared_down):
    num_seqs = hidden_in.shape[0]
    normed = rms_scale(hidden_in, attn_gain, eps_norm).astype(jnp.bfloat16)
    q_raw = jnp.dot(normed, query_w, preferred_element_type=jnp.float32)
    k_raw = jnp.dot(normed, key_w, preferred_element_type=jnp.float32)
    value_new = jnp.dot(normed, value_w, preferred_element_type=jnp.float32).astype(jnp.bfloat16)
    queries = rotate(q_raw.reshape(num_seqs, KV_HEADS, -1, 2, HEAD_DIM), lengths[:, None, None, None]).astype(jnp.bfloat16)
    key_new = rotate(k_raw.reshape(num_seqs, KV_HEADS, 2, HEAD_DIM), lengths[:, None, None]).astype(jnp.bfloat16)

    def one_sequence(items):
        return attend(*[item[None] for item in items], lam_heads, head_gain)[0]
    attn_out = lax.map(one_sequence, (queries, key_new, value_new, key_cache, value_cache, lengths))
    attn_proj = jnp.dot(attn_out, out_w, preferred_element_type=jnp.float32).astype(jnp.bfloat16)
    after_mixer = (hidden_in.astype(jnp.float32) + attn_proj.astype(jnp.float32)).astype(jnp.bfloat16)
    moe_in = rms_scale(after_mixer, moe_gain, eps_norm).astype(jnp.bfloat16)
    routed = routed_sum(moe_in, routing, route_weight, gate_w, up_w, down_w)
    shared_hidden = (jax.nn.silu(jnp.dot(moe_in, shared_gate, preferred_element_type=jnp.float32)) * jnp.dot(moe_in, shared_up, preferred_element_type=jnp.float32)).astype(jnp.bfloat16)
    shared_out = jnp.dot(shared_hidden, shared_down, preferred_element_type=jnp.float32)
    layer_out = (after_mixer.astype(jnp.float32) + routed + shared_out).astype(jnp.bfloat16)
    return (layer_out, key_new.reshape(num_seqs, -1), value_new)
```

```python
import functools

import jax
import jax.numpy as jnp
import numpy as np
from jax import lax
from jax.experimental import pallas as pl
from jax.experimental.pallas import tpu as pltpu
from jax.sharding import PartitionSpec as P

KV_HEADS = 2
HEAD_DIM = 128
LANES = 128

eps_norm = 1e-06
eps_head = 1e-05
theta_base = 500000.0

MESH = pl.DeviceIdType.MESH
f32 = jnp.float32
bf16 = jnp.bfloat16


def inv_rms(rows, epsilon):
    return lax.rsqrt(jnp.mean(rows * rows, axis=-1, keepdims=True) + epsilon)


def wait_bytes(ref, sem):
    pltpu.make_async_copy(ref, ref, sem).wait()


def layer_kernel(
    n,
    lengths,
    lam,
    hidden_hbm,
    keys_hbm,
    values_hbm,
    qw_hbm,
    kw_hbm,
    vw_hbm,
    ow_hbm,
    gate_hbm,
    up_hbm,
    down_hbm,
    sgate_hbm,
    sup_hbm,
    sdown_hbm,
    head_gain,
    attn_gain,
    moe_gain,
    routing,
    route_weight,
    freqs,
    out_ref,
    key_out,
    value_out,
    hid,
    w_in,
    w_out,
    keys,
    values,
    gate,
    up,
    down,
    sgate,
    sup,
    sdown,
    gat,
    wq,
    wo,
    rows32,
    rows16,
    csum,
    proj,
    abuf,
    att,
    obuf,
    cols,
    hbuf,
    res,
    ebuf,
    back,
    local_sem,
    send_sem,
    recv_sem,
    tile_sem,
):
    me = lax.axis_index("ep")
    tok, width = hid.shape
    rows = w_in.shape[0]
    in_tiles, out_tiles = proj.shape[0], cols.shape[0]
    q_tiles = qw_hbm.shape[1] // LANES
    k_tiles = kw_hbm.shape[1] // LANES
    group = q_tiles // (2 * KV_HEADS)
    total = n * tok
    peers_step = 16 // tok

    def load(src, dst, i):
        copy = pltpu.make_async_copy(src, dst, local_sem.at[i])
        copy.start()
        return copy

    def put(src, dst, phase, target, sent=None):
        pltpu.make_async_remote_copy(
            src_ref=src,
            dst_ref=dst,
            send_sem=send_sem.at[phase] if sent is None else sent,
            recv_sem=recv_sem.at[phase],
            device_id=(target,),
            device_id_type=MESH,
        ).start()

    def keep(src, dst, phase):
        pltpu.make_async_copy(src, dst, recv_sem.at[phase]).start()

    def put_or_keep(src, dst, phase, target):
        @pl.when(target != me)
        def _():
            put(src, dst, phase, target)

        @pl.when(target == me)
        def _():
            keep(src, dst, phase)

    def each_peer(body):
        def step(k, carry):
            body(lax.rem(me + k, n))
            return carry

        lax.fori_loop(1, n, step, 0)

    q_width, k_width = qw_hbm.shape[1], kw_hbm.shape[1]
    first = [
        load(hidden_hbm, hid, 0),
        load(qw_hbm, w_in.at[:, pl.ds(0, q_width)], 1),
        load(kw_hbm, w_in.at[:, pl.ds(q_width, k_width)], 2),
        load(vw_hbm, w_in.at[:, pl.ds(q_width + k_width, vw_hbm.shape[1])], 3),
        load(ow_hbm, w_out, 4),
    ]
    barrier = pltpu.get_barrier_semaphore()
    each_peer(
        lambda p: pl.semaphore_signal(barrier, inc=1, device_id=(p,), device_id_type=MESH)
    )
    load_keys = load(keys_hbm, keys, 5)
    load_values = load(values_hbm, values, 6)
    load_gate = load(gate_hbm.at[0], gate, 7)
    load_up = load(up_hbm.at[0], up, 8)
    load_down = load(down_hbm.at[0], down, 9)
    load_sgate = load(sgate_hbm, sgate, 10)
    load_sup = load(sup_hbm, sup, 11)
    load_sdown = load(sdown_hbm, sdown, 12)
    for copy in first:
        copy.wait()
    pl.semaphore_wait(barrier, n - 1)

    each_peer(lambda p: put(hid, gat.at[me], 0, p))
    keep(hid, gat.at[me], 0)
    own_rows = pl.ds(pl.multiple_of(me * rows, rows), rows)
    in_owner = lambda c: (c * n) // in_tiles
    stride = n // out_tiles
    out_owner = lambda c: c * stride + stride - 1

    def send_in(k, carry):
        c = lax.rem(k + me, in_tiles)
        cols_c = pl.ds(pl.multiple_of(c * LANES, LANES), LANES)
        put_or_keep(w_in.at[:, cols_c], wq.at[own_rows, :], 1, in_owner(c))
        return carry

    lax.fori_loop(0, in_tiles, send_in, 0)

    def send_out(k, carry):
        c = lax.rem(k + me, out_tiles)
        cols_c = pl.ds(pl.multiple_of(c * LANES, LANES), LANES)
        put_or_keep(w_out.at[:, cols_c], wo.at[own_rows, :], 2, out_owner(c))
        return carry

    lax.fori_loop(0, out_tiles, send_out, 0)
    my_in = (me * in_tiles + n - 1) // n
    has_in = in_owner(my_in) == me
    my_out = me // stride
    has_out = lax.rem(me, stride) == stride - 1

    def stacked(buf, i):
        return jnp.concatenate(
            [buf[i * peers_step + k].astype(f32) for k in range(peers_step)], axis=0
        )

    wait_bytes(gat, recv_sem.at[0])

    def norm_rows(i, carry):
        x = stacked(gat, i)
        at = pl.ds(pl.multiple_of(i * 16, 16), 16)
        rows32[at, :] = x
        rows16[at, :] = (x * inv_rms(x, eps_norm) * attn_gain[...]).astype(bf16)
        return carry

    lax.fori_loop(0, total // 16, norm_rows, 0)

    @pl.when(has_in)
    def _():
        wait_bytes(wq, recv_sem.at[1])
        sums = jnp.dot(rows16[...], wq[...], preferred_element_type=f32)
        for p in range(n):
            csum[p] = sums[p * tok : (p + 1) * tok, :]
        each_peer(lambda p: put(csum.at[p], proj.at[my_in], 3, p))
        keep(csum.at[me], proj.at[my_in], 3)

    row_id = lax.broadcasted_iota(jnp.int32, (tok, LANES), 0)
    position = jnp.zeros((tok, LANES), jnp.int32)
    for s in range(tok):
        position = jnp.where(row_id == s, lengths[s], position)
    angle = position.astype(f32) * freqs[...]
    cosine, sine = jnp.cos(angle), jnp.sin(angle)
    low = lax.broadcasted_iota(jnp.int32, (tok, LANES), 1) < LANES // 2
    sine = jnp.where(low, -sine, sine)
    load_keys.wait()
    load_values.wait()
    wait_bytes(proj, recv_sem.at[3])
    turned = []
    for c in range(q_tiles + k_tiles):
        x = proj[c]
        turned.append((x * cosine + pltpu.roll(x, LANES // 2, 1) * sine).astype(bf16).astype(f32))
    new_values = [proj[c].astype(bf16).astype(f32) for c in range(q_tiles + k_tiles, in_tiles)]
    key_out[...] = jnp.concatenate(turned[q_tiles:], axis=1).astype(bf16)
    value_out[...] = jnp.concatenate(new_values, axis=1).astype(bf16)
    v_tiles = len(new_values) // KV_HEADS

    cache_len = keys.shape[1]
    scale = HEAD_DIM ** (-0.5)
    pairs = 2 * group
    value_dim = v_tiles * LANES
    first_map = lax.broadcasted_iota(jnp.int32, (pairs, cache_len), 0) < group
    spot = lax.broadcasted_iota(jnp.int32, (pairs, cache_len), 1)
    contract = (((1,), (1,)), ((), ()))
    out_rows = []
    for s in range(tok):
        heads = []
        for kv in range(KV_HEADS):
            q = jnp.concatenate(
                [
                    turned[(kv * group + g) * 2 + j][s : s + 1]
                    for j in range(2)
                    for g in range(group)
                ],
                axis=0,
            )
            own_key = jnp.concatenate(
                [turned[q_tiles + kv * 2 + j][s : s + 1] for j in range(2) for g in range(group)],
                axis=0,
            )
            q16 = q.astype(bf16)
            parts = [
                lax.dot_general(
                    q16,
                    keys[s, :, (kv * 2 + j) * LANES : (kv * 2 + j + 1) * LANES],
                    contract,
                    preferred_element_type=f32,
                )
                for j in range(2)
            ]
            live = spot < lengths[s]
            scores = jnp.where(live, jnp.where(first_map, parts[0], parts[1]) * scale, -jnp.inf)
            self_score = jnp.sum(q * own_key, axis=1, keepdims=True) * scale
            peak = jnp.maximum(jnp.max(scores, axis=1, keepdims=True), self_score)
            weights = jnp.exp(scores - peak)
            self_weight = jnp.exp(self_score - peak)
            totals = jnp.sum(weights, axis=1, keepdims=True) + self_weight
            map_row = lax.broadcasted_iota(jnp.int32, (pairs, 1), 0)
            factor = jnp.ones((pairs, 1), f32)
            for g in range(group):
                factor = jnp.where(map_row == group + g, lam[kv * group + g], factor)
            factor = factor / totals
            scaled = weights * factor
            self_scaled = jnp.broadcast_to(self_weight * factor, (pairs, LANES))
            combined = (scaled[:group] - scaled[group:]).astype(bf16)
            self_comb = (self_scaled[:group] - self_scaled[group:]).astype(bf16).astype(f32)
            head = jnp.dot(
                combined,
                values[s, :, kv * value_dim : (kv + 1) * value_dim],
                preferred_element_type=f32,
            )
            own_value = jnp.concatenate(
                [new_values[kv * v_tiles + v][s : s + 1] for v in range(v_tiles)], axis=1
            )
            head = head + self_comb[:, :1] * own_value
            head = head * inv_rms(head, eps_head) * head_gain[...]
            heads += [head[g : g + 1] for g in range(group)]
        out_rows.append(jnp.concatenate(heads, axis=1))
    abuf[...] = jnp.concatenate(out_rows, axis=0).astype(bf16)

    def send_att(k, carry):
        put_or_keep(abuf, att.at[me], 4, out_owner(lax.rem(k + my_out, out_tiles)))
        return carry

    lax.fori_loop(0, out_tiles, send_att, 0)

    @pl.when(has_out)
    def _():
        wait_bytes(wo, recv_sem.at[2])
        wait_bytes(att, recv_sem.at[4])

        def stack_rows(i, carry):
            rows16[pl.ds(pl.multiple_of(i * 16, 16), 16), :] = stacked(att, i).astype(bf16)
            return carry

        lax.fori_loop(0, total // 16, stack_rows, 0)
        obuf[...] = jnp.dot(rows16[...], wo[...], preferred_element_type=f32).astype(bf16)
        each_peer(lambda p: put(obuf, cols.at[my_out], 5, p, tile_sem.at[p]))
        keep(obuf, cols.at[my_out], 5)

    wait_bytes(cols, recv_sem.at[5])

    def mix_rows(i, carry):
        at = pl.ds(pl.multiple_of(i * 16, 16), 16)
        added = jnp.concatenate([cols[c, at, :] for c in range(out_tiles)], axis=1)
        x = (rows32[at, :] + added.astype(f32)).astype(bf16).astype(f32)
        rows32[at, :] = x
        rows16[at, :] = (x * inv_rms(x, eps_norm) * moe_gain[...]).astype(bf16)
        return carry

    lax.fori_loop(0, total // 16, mix_rows, 0)
    load_gate.wait()
    load_up.wait()
    load_down.wait()

    def hide(block, gate_w, up_w, at):
        g = jnp.dot(block, gate_w[:, at], preferred_element_type=f32)
        u = jnp.dot(block, up_w[:, at], preferred_element_type=f32)
        return (g * jax.nn.sigmoid(g) * u).astype(bf16)

    chunk = 256
    for c in range(gate.shape[1] // chunk):
        at = slice(c * chunk, (c + 1) * chunk)
        hbuf[:, at] = hide(rows16[...], gate, up, at)
    for c in range(width // chunk):
        at = slice(c * chunk, (c + 1) * chunk)
        res[:, at] = jnp.dot(hbuf[...], down[:, at], preferred_element_type=f32)

    def split_rows(i, carry):
        block = res[pl.ds(pl.multiple_of(i * 16, 16), 16), :]
        for k in range(peers_step):
            ebuf[i * peers_step + k] = block[k * tok : (k + 1) * tok, :].astype(bf16)
        return carry

    lax.fori_loop(0, total // 16, split_rows, 0)
    each_peer(lambda p: put(ebuf.at[p], back.at[me], 6, p))
    keep(ebuf.at[me], back.at[me], 6)

    load_sgate.wait()
    load_sup.wait()
    load_sdown.wait()
    per_block = 8 // tok

    def own(ref):
        block = ref[pl.ds(pl.multiple_of(me // per_block * 8, 8), 8), :]
        picked = block[:tok]
        for k in range(1, per_block):
            here = lax.rem(me, per_block) == k
            picked = jnp.where(here, block[k * tok : (k + 1) * tok], picked)
        return picked

    after_mixer = own(rows32)
    moe_in = (after_mixer * inv_rms(after_mixer, eps_norm) * moe_gain[...]).astype(bf16)
    shared_hidden = jnp.concatenate(
        [
            hide(moe_in, sgate, sup, slice(c * chunk, (c + 1) * chunk))
            for c in range(sgate.shape[1] // chunk)
        ],
        axis=1,
    )
    shared_out = jnp.concatenate(
        [
            jnp.dot(
                shared_hidden,
                sdown[:, c * chunk : (c + 1) * chunk],
                preferred_element_type=f32,
            )
            for c in range(width // chunk)
        ],
        axis=1,
    )
    named = own(routing)
    named_weight = own(route_weight)
    expert_id = lax.broadcasted_iota(jnp.int32, (tok, n), 1)
    table = jnp.zeros((tok, n), f32)
    for k in range(named.shape[1]):
        table = table + jnp.where(
            expert_id == named[:, k : k + 1], named_weight[:, k : k + 1], 0.0
        )
    wait_bytes(back, recv_sem.at[6])
    routed = jnp.zeros((tok, width), f32)
    for e in range(n):
        routed = routed + table[:, e : e + 1] * back[e].astype(f32)
    out_ref[...] = (after_mixer + routed + shared_out).astype(bf16)

    others = pl.ds(0, n - 1)
    wait_bytes(gat.at[others], send_sem.at[0])
    wait_bytes(back.at[others], send_sem.at[6])

    def drain(mine, some, every, phase):
        @pl.when(mine)
        def _():
            wait_bytes(some, send_sem.at[phase])

        @pl.when(jnp.logical_not(mine))
        def _():
            wait_bytes(every, send_sem.at[phase])

    drain(has_in, w_in.at[:, pl.ds(0, (in_tiles - 1) * LANES)], w_in, 1)
    drain(has_out, w_out.at[:, pl.ds(0, (out_tiles - 1) * LANES)], w_out, 2)
    drain(has_out, att.at[pl.ds(0, out_tiles - 1)], att.at[pl.ds(0, out_tiles)], 4)

    @pl.when(has_in)
    def _():
        wait_bytes(csum.at[others], send_sem.at[3])

    @pl.when(has_out)
    def _():
        each_peer(lambda p: wait_bytes(obuf, tile_sem.at[p]))


def on_device(
    n,
    hidden_in,
    lengths,
    key_cache,
    value_cache,
    query_w,
    key_w,
    value_w,
    out_w,
    lam_heads,
    head_gain,
    attn_gain,
    moe_gain,
    routing,
    route_weight,
    gate_w,
    up_w,
    down_w,
    shared_gate,
    shared_up,
    shared_down,
):
    tok, width = hidden_in.shape
    total = n * tok
    rows = query_w.shape[0]
    in_width = query_w.shape[1] + key_w.shape[1] + value_w.shape[1]
    in_tiles, out_tiles = in_width // LANES, width // LANES
    half = HEAD_DIM // 2
    inverse = np.power(theta_base, -np.arange(half) / half).astype(np.float32)
    freqs = jnp.asarray(np.concatenate([inverse, inverse])[None, :])
    smem = pl.BlockSpec(memory_space=pltpu.SMEM)
    vmem = pl.BlockSpec(memory_space=pltpu.VMEM)
    hbm = pl.BlockSpec(memory_space=pl.ANY)
    like = lambda a: pltpu.VMEM(a.shape, a.dtype)
    return pl.pallas_call(
        functools.partial(layer_kernel, n),
        out_shape=(
            jax.ShapeDtypeStruct((tok, width), bf16),
            jax.ShapeDtypeStruct((tok, key_w.shape[1]), bf16),
            jax.ShapeDtypeStruct((tok, value_w.shape[1]), bf16),
        ),
        in_specs=[smem] * 2 + [hbm] * 13 + [vmem] * 6,
        out_specs=(vmem, vmem, vmem),
        scratch_shapes=[
            like(hidden_in),
            pltpu.VMEM((rows, in_width), bf16),
            like(out_w),
            like(key_cache),
            like(value_cache),
            pltpu.VMEM(gate_w.shape[1:], bf16),
            pltpu.VMEM(up_w.shape[1:], bf16),
            pltpu.VMEM(down_w.shape[1:], bf16),
            like(shared_gate),
            like(shared_up),
            like(shared_down),
            pltpu.VMEM((n, tok, width), bf16),
            pltpu.VMEM((n * rows, LANES), bf16),
            pltpu.VMEM((n * out_w.shape[0], LANES), bf16),
            pltpu.VMEM((total, width), f32),
            pltpu.VMEM((total, width), bf16),
            pltpu.VMEM((n, tok, LANES), f32),
            pltpu.VMEM((in_tiles, tok, LANES), f32),
            pltpu.VMEM((tok, width), bf16),
            pltpu.VMEM((n, tok, width), bf16),
            pltpu.VMEM((total, LANES), bf16),
            pltpu.VMEM((out_tiles, total, LANES), bf16),
            pltpu.VMEM((total, gate_w.shape[2]), bf16),
            pltpu.VMEM((total, width), f32),
            pltpu.VMEM((n, tok, width), bf16),
            pltpu.VMEM((n, tok, width), bf16),
            pltpu.SemaphoreType.DMA((13,)),
            pltpu.SemaphoreType.DMA((7,)),
            pltpu.SemaphoreType.DMA((7,)),
            pltpu.SemaphoreType.DMA((n,)),
        ],
        compiler_params=pltpu.CompilerParams(
            collective_id=0, has_side_effects=True, vmem_limit_bytes=64000000
        ),
        name="decode_layer",
    )(
        lengths,
        lam_heads,
        hidden_in,
        key_cache,
        value_cache,
        query_w,
        key_w,
        value_w,
        out_w,
        gate_w,
        up_w,
        down_w,
        shared_gate,
        shared_up,
        shared_down,
        head_gain[None, :],
        attn_gain[None, :],
        moe_gain[None, :],
        routing,
        route_weight,
        freqs,
    )


def solution(mesh):
    placed = (
        P("ep", None),
        P("ep"),
        P("ep", None, None),
        P("ep", None, None),
        P("ep", None),
        P("ep", None),
        P("ep", None),
        P("ep", None),
        P(),
        P(),
        P(),
        P(),
        P(),
        P(),
        P("ep", None, None),
        P("ep", None, None),
        P("ep", None, None),
        P(),
        P(),
        P(),
    )
    return jax.shard_map(
        functools.partial(on_device, mesh.shape["ep"]),
        mesh=mesh,
        in_specs=placed,
        out_specs=(P("ep", None), P("ep", None), P("ep", None)),
        check_vma=False,
    )
```

```python
import functools
import math

import jax
import jax.numpy as jnp
import numpy as np
from jax import lax
from jax.experimental import pallas as pl
from jax.experimental.pallas import tpu as pltpu
from jax.sharding import PartitionSpec as P

KV_HEADS = 2
HEAD_DIM = 128
LANES = 128

eps_norm = 1e-06
eps_head = 1e-05
theta_base = 500000.0

MESH = pl.DeviceIdType.MESH
f32 = jnp.float32
bf16 = jnp.bfloat16


def inv_rms(rows, epsilon):
    return lax.rsqrt(jnp.mean(rows * rows, axis=-1, keepdims=True) + epsilon)


def wait_bytes(ref, sem):
    pltpu.make_async_copy(ref, ref, sem).wait()


def layer_kernel(
    n,
    lengths,
    lam,
    hidden_hbm,
    keys_hbm,
    values_hbm,
    qw_hbm,
    kw_hbm,
    vw_hbm,
    ow_hbm,
    gate_hbm,
    up_hbm,
    down_hbm,
    sgate_hbm,
    sup_hbm,
    sdown_hbm,
    head_gain,
    attn_gain,
    moe_gain,
    routing,
    route_weight,
    freqs,
    out_ref,
    key_out,
    value_out,
    hid,
    w_in,
    w_out,
    keys,
    values,
    gate,
    up,
    down,
    sgate,
    sup,
    sdown,
    nbuf,
    xin,
    wq,
    wo,
    xrows,
    csum,
    proj,
    abuf,
    att,
    osum,
    oproj,
    mbuf,
    gat,
    rows16,
    hbuf,
    res,
    ebuf,
    back,
    local_sem,
    send_sem,
    recv_sem,
):
    me = lax.axis_index("ep")
    tok, width = hid.shape
    rows = w_in.shape[0]
    in_block, out_block = wq.shape[1], wo.shape[1]
    depth = wq.shape[0]
    size = depth // rows
    blocks = n // size
    in_tiles = size * in_block // LANES
    q_tiles = qw_hbm.shape[1] // LANES
    k_tiles = kw_hbm.shape[1] // LANES
    group = q_tiles // (2 * KV_HEADS)
    total = n * tok
    peers_step = 16 // tok

    def load(src, dst, i):
        copy = pltpu.make_async_copy(src, dst, local_sem.at[i])
        copy.start()
        return copy

    def put(src, dst, phase, target):
        pltpu.make_async_remote_copy(
            src_ref=src,
            dst_ref=dst,
            send_sem=send_sem.at[phase],
            recv_sem=recv_sem.at[phase],
            device_id=(target,),
            device_id_type=MESH,
        ).start()

    def keep(src, dst, phase):
        pltpu.make_async_copy(src, dst, recv_sem.at[phase]).start()

    def each_peer(body):
        def step(k, carry):
            body(lax.rem(me + k, n))
            return carry

        lax.fori_loop(1, n, step, 0)

    q_width, k_width = qw_hbm.shape[1], kw_hbm.shape[1]
    first = [
        load(hidden_hbm, hid, 0),
        load(qw_hbm, w_in.at[:, pl.ds(0, q_width)], 1),
        load(kw_hbm, w_in.at[:, pl.ds(q_width, k_width)], 2),
        load(vw_hbm, w_in.at[:, pl.ds(q_width + k_width, vw_hbm.shape[1])], 3),
        load(ow_hbm, w_out, 4),
    ]
    barrier = pltpu.get_barrier_semaphore()
    each_peer(
        lambda p: pl.semaphore_signal(barrier, inc=1, device_id=(p,), device_id_type=MESH)
    )
    load_keys = load(keys_hbm, keys, 5)
    load_values = load(values_hbm, values, 6)
    load_gate = load(gate_hbm.at[0], gate, 7)
    load_up = load(up_hbm.at[0], up, 8)
    load_down = load(down_hbm.at[0], down, 9)
    load_sgate = load(sgate_hbm, sgate, 10)
    load_sup = load(sup_hbm, sup, 11)
    load_sdown = load(sdown_hbm, sdown, 12)
    first[0].wait()
    x = hid[...].astype(f32)
    normed = (x * inv_rms(x, eps_norm) * attn_gain[...]).astype(bf16)
    for b in range(blocks):
        nbuf[b] = normed[:, b * depth : (b + 1) * depth]
    for copy in first[1:]:
        copy.wait()
    pl.semaphore_wait(barrier, n - 1)

    each_peer(lambda p: put(nbuf.at[p // size], xin.at[me], 0, p))
    keep(nbuf.at[me // size], xin.at[me], 0)
    place = lax.rem(me, size)
    own_rows = pl.ds(pl.multiple_of(place * rows, rows), rows)

    def share(weights, block, dst, phase):
        def part(q):
            return weights.at[:, pl.ds(pl.multiple_of(q * block, block), block)]

        def step(k, carry):
            q = lax.rem(place + k, size)
            put(part(q), dst.at[own_rows, :], phase, me - place + q)
            return carry

        lax.fori_loop(1, size, step, 0)
        keep(part(place), dst.at[own_rows, :], phase)

    share(w_in, in_block, wq, 1)
    share(w_out, out_block, wo, 2)

    def stacked(buf, i):
        return jnp.concatenate(
            [buf[i * peers_step + k].astype(f32) for k in range(peers_step)], axis=0
        ).astype(bf16)

    def stack(buf, dst):
        def step(i, carry):
            dst[pl.ds(pl.multiple_of(i * 16, 16), 16), :] = stacked(buf, i)
            return carry

        lax.fori_loop(0, total // 16, step, 0)

    def project(buf, weights, sums, dst, phase):
        stack(buf, xrows)
        part = jnp.dot(xrows[...], weights[...], preferred_element_type=f32)
        for p in range(n):
            sums[p] = part[p * tok : (p + 1) * tok, :]
        each_peer(lambda p: put(sums.at[p], dst.at[me], phase, p))
        keep(sums.at[me], dst.at[me], phase)

    wait_bytes(xin, recv_sem.at[0])
    wait_bytes(wq, recv_sem.at[1])
    project(xin, wq, csum, proj, 3)

    row_id = lax.broadcasted_iota(jnp.int32, (tok, LANES), 0)
    position = jnp.zeros((tok, LANES), jnp.int32)
    for s in range(tok):
        position = jnp.where(row_id == s, lengths[s], position)
    angle = position.astype(f32) * freqs[...]
    cosine, sine = jnp.cos(angle), jnp.sin(angle)
    low = lax.broadcasted_iota(jnp.int32, (tok, LANES), 1) < LANES // 2
    sine = jnp.where(low, -sine, sine)
    load_keys.wait()
    load_values.wait()
    wait_bytes(proj, recv_sem.at[3])

    def summed(buf, q):
        whole = buf[q]
        for b in range(1, blocks):
            whole = whole + buf[b * size + q]
        return whole

    projected = jnp.concatenate([summed(proj, q) for q in range(size)], axis=1)
    tiles = [projected[:, c * LANES : (c + 1) * LANES] for c in range(in_tiles)]
    turned = []
    for c in range(q_tiles + k_tiles):
        x = tiles[c]
        turned.append((x * cosine + pltpu.roll(x, LANES // 2, 1) * sine).astype(bf16).astype(f32))
    new_values = [tiles[c].astype(bf16).astype(f32) for c in range(q_tiles + k_tiles, in_tiles)]
    key_out[...] = jnp.concatenate(turned[q_tiles:], axis=1).astype(bf16)
    value_out[...] = jnp.concatenate(new_values, axis=1).astype(bf16)
    v_tiles = len(new_values) // KV_HEADS

    cache_len = keys.shape[1]
    scale = HEAD_DIM ** (-0.5)
    pairs = 2 * group
    value_dim = v_tiles * LANES
    first_map = lax.broadcasted_iota(jnp.int32, (pairs, cache_len), 0) < group
    spot = lax.broadcasted_iota(jnp.int32, (pairs, cache_len), 1)
    contract = (((1,), (1,)), ((), ()))
    out_rows = []
    for s in range(tok):
        heads = []
        for kv in range(KV_HEADS):
            q = jnp.concatenate(
                [
                    turned[(kv * group + g) * 2 + j][s : s + 1]
                    for j in range(2)
                    for g in range(group)
                ],
                axis=0,
            )
            own_key = jnp.concatenate(
                [turned[q_tiles + kv * 2 + j][s : s + 1] for j in range(2) for g in range(group)],
                axis=0,
            )
            q16 = q.astype(bf16)
            parts = [
                lax.dot_general(
                    q16,
                    keys[s, :, (kv * 2 + j) * LANES : (kv * 2 + j + 1) * LANES],
                    contract,
                    preferred_element_type=f32,
                )
                for j in range(2)
            ]
            live = spot < lengths[s]
            scores = jnp.where(live, jnp.where(first_map, parts[0], parts[1]) * scale, -jnp.inf)
            self_score = jnp.sum(q * own_key, axis=1, keepdims=True) * scale
            peak = jnp.maximum(jnp.max(scores, axis=1, keepdims=True), self_score)
            weights = jnp.exp(scores - peak)
            self_weight = jnp.exp(self_score - peak)
            totals = jnp.sum(weights, axis=1, keepdims=True) + self_weight
            map_row = lax.broadcasted_iota(jnp.int32, (pairs, 1), 0)
            factor = jnp.ones((pairs, 1), f32)
            for g in range(group):
                factor = jnp.where(map_row == group + g, lam[kv * group + g], factor)
            factor = factor / totals
            scaled = weights * factor
            self_scaled = jnp.broadcast_to(self_weight * factor, (pairs, LANES))
            combined = (scaled[:group] - scaled[group:]).astype(bf16)
            self_comb = (self_scaled[:group] - self_scaled[group:]).astype(bf16).astype(f32)
            head = jnp.dot(
                combined,
                values[s, :, kv * value_dim : (kv + 1) * value_dim],
                preferred_element_type=f32,
            )
            own_value = jnp.concatenate(
                [new_values[kv * v_tiles + v][s : s + 1] for v in range(v_tiles)], axis=1
            )
            head = head + self_comb[:, :1] * own_value
            head = head * inv_rms(head, eps_head) * head_gain[...]
            heads += [head[g : g + 1] for g in range(group)]
        out_rows.append(jnp.concatenate(heads, axis=1))
    attended = jnp.concatenate(out_rows, axis=0).astype(bf16)
    for b in range(blocks):
        abuf[b] = attended[:, b * depth : (b + 1) * depth]
    each_peer(lambda p: put(abuf.at[p // size], att.at[me], 4, p))
    keep(abuf.at[me // size], att.at[me], 4)

    wait_bytes(wo, recv_sem.at[2])
    wait_bytes(att, recv_sem.at[4])
    project(att, wo, osum, oproj, 5)
    wait_bytes(oproj, recv_sem.at[5])
    attn_proj = jnp.concatenate([summed(oproj, q) for q in range(size)], axis=1)
    after_mixer = hid[...].astype(f32) + attn_proj.astype(bf16).astype(f32)
    after_mixer = after_mixer.astype(bf16).astype(f32)
    moe_in = (after_mixer * inv_rms(after_mixer, eps_norm) * moe_gain[...]).astype(bf16)
    mbuf[...] = moe_in
    each_peer(lambda p: put(mbuf, gat.at[me], 6, p))
    keep(mbuf, gat.at[me], 6)
    wait_bytes(gat, recv_sem.at[6])
    stack(gat, rows16)
    load_gate.wait()
    load_up.wait()
    load_down.wait()

    def hide(block, gate_w, up_w, at):
        g = jnp.dot(block, gate_w[:, at], preferred_element_type=f32)
        u = jnp.dot(block, up_w[:, at], preferred_element_type=f32)
        return (g * jax.nn.sigmoid(g) * u).astype(bf16)

    chunk = 256
    for c in range(gate.shape[1] // chunk):
        at = slice(c * chunk, (c + 1) * chunk)
        hbuf[:, at] = hide(rows16[...], gate, up, at)
    for c in range(width // chunk):
        at = slice(c * chunk, (c + 1) * chunk)
        res[:, at] = jnp.dot(hbuf[...], down[:, at], preferred_element_type=f32)

    def split_rows(i, carry):
        block = res[pl.ds(pl.multiple_of(i * 16, 16), 16), :]
        for k in range(peers_step):
            ebuf[i * peers_step + k] = block[k * tok : (k + 1) * tok, :].astype(bf16)
        return carry

    lax.fori_loop(0, total // 16, split_rows, 0)
    each_peer(lambda p: put(ebuf.at[p], back.at[me], 7, p))
    keep(ebuf.at[me], back.at[me], 7)

    load_sgate.wait()
    load_sup.wait()
    load_sdown.wait()
    shared_hidden = jnp.concatenate(
        [
            hide(moe_in, sgate, sup, slice(c * chunk, (c + 1) * chunk))
            for c in range(sgate.shape[1] // chunk)
        ],
        axis=1,
    )
    shared_out = jnp.concatenate(
        [
            jnp.dot(
                shared_hidden,
                sdown[:, c * chunk : (c + 1) * chunk],
                preferred_element_type=f32,
            )
            for c in range(width // chunk)
        ],
        axis=1,
    )
    tokens, places = routing[...].astype(f32), route_weight[...]
    column = lax.broadcasted_iota(jnp.int32, tokens.shape, 1)
    expert_id = lax.broadcasted_iota(jnp.int32, (tokens.shape[0], n), 1).astype(f32)
    lines = []
    for s in range(tok):
        here = column == me * tok + s
        named = jnp.sum(jnp.where(here, tokens, 0.0), axis=1, keepdims=True)
        weight = jnp.sum(jnp.where(here, places, 0.0), axis=1, keepdims=True)
        chosen = jnp.where(expert_id == named, weight, 0.0)
        lines.append(jnp.sum(chosen, axis=0, keepdims=True))
    table = jnp.concatenate(lines, axis=0)
    wait_bytes(back, recv_sem.at[7])
    routed = jnp.zeros((tok, width), f32)
    for e in range(n):
        routed = routed + table[:, e : e + 1] * back[e].astype(f32)
    out_ref[...] = (after_mixer + routed + shared_out).astype(bf16)

    others, mates = pl.ds(0, n - 1), pl.ds(0, depth - rows)
    sent = (xin.at[others], wq.at[mates], wo.at[mates], proj.at[others])
    sent += (att.at[others], oproj.at[others], gat.at[others], back.at[others])
    for phase, ref in enumerate(sent):
        wait_bytes(ref, send_sem.at[phase])


def hand_on(*refs):
    for source, target in zip(refs[:3], refs[3:]):
        target[...] = source[...]


def on_device(
    n,
    hidden_in,
    lengths,
    key_cache,
    value_cache,
    query_w,
    key_w,
    value_w,
    out_w,
    lam_heads,
    head_gain,
    attn_gain,
    moe_gain,
    routing,
    route_weight,
    gate_w,
    up_w,
    down_w,
    shared_gate,
    shared_up,
    shared_down,
):
    tok, width = hidden_in.shape
    total = n * tok
    rows = query_w.shape[0]
    in_width = query_w.shape[1] + key_w.shape[1] + value_w.shape[1]
    size = math.gcd(in_width // LANES, width // LANES)
    depth = size * rows
    in_block, out_block = in_width // size, width // size
    half = HEAD_DIM // 2
    inverse = np.power(theta_base, -np.arange(half) / half).astype(np.float32)
    freqs = jnp.asarray(np.concatenate([inverse, inverse])[None, :])
    smem = pl.BlockSpec(memory_space=pltpu.SMEM)
    vmem = pl.BlockSpec(memory_space=pltpu.VMEM)
    hbm = pl.BlockSpec(memory_space=pl.ANY)
    like = lambda a: pltpu.VMEM(a.shape, a.dtype)
    shapes = (
        jax.ShapeDtypeStruct((tok, width), bf16),
            jax.ShapeDtypeStruct((tok, key_w.shape[1]), bf16),
            jax.ShapeDtypeStruct((tok, value_w.shape[1]), bf16),
    )
    results = pl.pallas_call(
        functools.partial(layer_kernel, n),
        out_shape=shapes,
        in_specs=[smem] * 2 + [hbm] * 13 + [vmem] * 6,
        out_specs=(vmem, vmem, vmem),
        scratch_shapes=[
            like(hidden_in),
            pltpu.VMEM((rows, in_width), bf16),
            like(out_w),
            like(key_cache),
            like(value_cache),
            pltpu.VMEM(gate_w.shape[1:], bf16),
            pltpu.VMEM(up_w.shape[1:], bf16),
            pltpu.VMEM(down_w.shape[1:], bf16),
            like(shared_gate),
            like(shared_up),
            like(shared_down),
            pltpu.VMEM((n // size, tok, depth), bf16),
            pltpu.VMEM((n, tok, depth), bf16),
            pltpu.VMEM((depth, in_block), bf16),
            pltpu.VMEM((depth, out_block), bf16),
            pltpu.VMEM((total, depth), bf16),
            pltpu.VMEM((n, tok, in_block), f32),
            pltpu.VMEM((n, tok, in_block), f32),
            pltpu.VMEM((n // size, tok, depth), bf16),
            pltpu.VMEM((n, tok, depth), bf16),
            pltpu.VMEM((n, tok, out_block), f32),
            pltpu.VMEM((n, tok, out_block), f32),
            pltpu.VMEM((tok, width), bf16),
            pltpu.VMEM((n, tok, width), bf16),
            pltpu.VMEM((total, width), bf16),
            pltpu.VMEM((total, gate_w.shape[2]), bf16),
            pltpu.VMEM((total, width), f32),
            pltpu.VMEM((n, tok, width), bf16),
            pltpu.VMEM((n, tok, width), bf16),
            pltpu.SemaphoreType.DMA((13,)),
            pltpu.SemaphoreType.DMA((8,)),
            pltpu.SemaphoreType.DMA((8,)),
        ],
        compiler_params=pltpu.CompilerParams(
            collective_id=0, has_side_effects=True, vmem_limit_bytes=64000000
        ),
        name="decode_layer",
    )(
        lengths,
        lam_heads,
        hidden_in,
        key_cache,
        value_cache,
        query_w,
        key_w,
        value_w,
        out_w,
        gate_w,
        up_w,
        down_w,
        shared_gate,
        shared_up,
        shared_down,
        head_gain[None, :],
        attn_gain[None, :],
        moe_gain[None, :],
        routing.T,
        route_weight.T,
        freqs,
    )
    return pl.pallas_call(
        hand_on,
        out_shape=shapes,
        in_specs=[vmem] * 3,
        out_specs=(vmem,) * 3,
        name="hand_on",
    )(*results)


def solution(mesh):
    placed = (
        P("ep", None),
        P("ep"),
        P("ep", None, None),
        P("ep", None, None),
        P("ep", None),
        P("ep", None),
        P("ep", None),
        P("ep", None),
        P(),
        P(),
        P(),
        P(),
        P(),
        P(),
        P("ep", None, None),
        P("ep", None, None),
        P("ep", None, None),
        P(),
        P(),
        P(),
    )
    return jax.shard_map(
        functools.partial(on_device, mesh.shape["ep"]),
        mesh=mesh,
        in_specs=placed,
        out_specs=(P("ep", None), P("ep", None), P("ep", None)),
        check_vma=False,
    )
```

```python
import functools
import math

import jax
import jax.numpy as jnp
import numpy as np
from jax import lax
from jax.experimental import pallas as pl
from jax.experimental.pallas import tpu as pltpu
from jax.sharding import PartitionSpec as P

KV_HEADS = 2
HEAD_DIM = 128
LANES = 128

eps_norm = 1e-06
eps_head = 1e-05
theta_base = 500000.0

MESH = pl.DeviceIdType.MESH
f32 = jnp.float32
bf16 = jnp.bfloat16


def inv_rms(rows, epsilon):
    return lax.rsqrt(jnp.mean(rows * rows, axis=-1, keepdims=True) + epsilon)


def wait_bytes(ref, sem):
    pltpu.make_async_copy(ref, ref, sem).wait()


def layer_kernel(
    n,
    lengths,
    lam,
    hidden_hbm,
    keys_hbm,
    values_hbm,
    qw_hbm,
    kw_hbm,
    vw_hbm,
    ow_hbm,
    gate_hbm,
    up_hbm,
    down_hbm,
    sgate_hbm,
    sup_hbm,
    sdown_hbm,
    head_gain,
    attn_gain,
    moe_gain,
    routing,
    route_weight,
    freqs,
    out_ref,
    key_out,
    value_out,
    hid,
    w_in,
    w_out,
    keys,
    values,
    gate,
    up,
    down,
    sgate,
    sup,
    sdown,
    nbuf,
    xin,
    wq,
    wo,
    xrows,
    csum,
    proj,
    abuf,
    att,
    osum,
    oproj,
    mbuf,
    gat,
    rows16,
    hbuf,
    res,
    ebuf,
    back,
    local_sem,
    send_sem,
    recv_sem,
    row_sem,
):
    me = lax.axis_index("ep")
    tok, width = hid.shape
    rows = w_in.shape[0]
    in_block, out_block = wq.shape[1], wo.shape[1]
    depth = wq.shape[0]
    size = depth // rows
    blocks = n // size
    in_tiles = size * in_block // LANES
    q_tiles = qw_hbm.shape[1] // LANES
    k_tiles = kw_hbm.shape[1] // LANES
    group = q_tiles // (2 * KV_HEADS)
    total = n * tok
    peers_step = 16 // tok

    def load(src, dst, i):
        copy = pltpu.make_async_copy(src, dst, local_sem.at[i])
        copy.start()
        return copy

    def put(src, dst, phase, target):
        pltpu.make_async_remote_copy(
            src_ref=src,
            dst_ref=dst,
            send_sem=send_sem.at[phase],
            recv_sem=recv_sem.at[phase],
            device_id=(target,),
            device_id_type=MESH,
        ).start()

    def keep(src, dst, phase):
        pltpu.make_async_copy(src, dst, recv_sem.at[phase]).start()

    def each_peer(body):
        def step(k, carry):
            body(lax.rem(me + k, n))
            return carry

        lax.fori_loop(1, n, step, 0)

    q_width, k_width = qw_hbm.shape[1], kw_hbm.shape[1]
    first = [
        load(hidden_hbm, hid, 0),
        load(qw_hbm, w_in.at[:, pl.ds(0, q_width)], 1),
        load(kw_hbm, w_in.at[:, pl.ds(q_width, k_width)], 2),
        load(vw_hbm, w_in.at[:, pl.ds(q_width + k_width, vw_hbm.shape[1])], 3),
        load(ow_hbm, w_out, 4),
    ]
    barrier = pltpu.get_barrier_semaphore()
    each_peer(
        lambda p: pl.semaphore_signal(barrier, inc=1, device_id=(p,), device_id_type=MESH)
    )
    load_keys = load(keys_hbm, keys, 5)
    load_values = load(values_hbm, values, 6)
    load_gate = load(gate_hbm.at[0], gate, 7)
    load_up = load(up_hbm.at[0], up, 8)
    load_down = load(down_hbm.at[0], down, 9)
    load_sgate = load(sgate_hbm, sgate, 10)
    load_sup = load(sup_hbm, sup, 11)
    load_sdown = load(sdown_hbm, sdown, 12)
    first[0].wait()
    x = hid[...].astype(f32)
    normed = (x * inv_rms(x, eps_norm) * attn_gain[...]).astype(bf16)
    for b in range(blocks):
        nbuf[b] = normed[:, b * depth : (b + 1) * depth]
    for copy in first[1:]:
        copy.wait()
    pl.semaphore_wait(barrier, n - 1)

    each_peer(lambda p: put(nbuf.at[p // size], xin.at[me], 0, p))
    keep(nbuf.at[me // size], xin.at[me], 0)
    place = lax.rem(me, size)
    own_rows = pl.ds(pl.multiple_of(place * rows, rows), rows)

    def share(weights, block, dst, phase):
        def part(q):
            return weights.at[:, pl.ds(pl.multiple_of(q * block, block), block)]

        def step(k, carry):
            q = lax.rem(place + k, size)
            put(part(q), dst.at[own_rows, :], phase, me - place + q)
            return carry

        lax.fori_loop(1, size, step, 0)
        keep(part(place), dst.at[own_rows, :], phase)

    share(w_in, in_block, wq, 1)
    share(w_out, out_block, wo, 2)

    def stacked(buf, i):
        return jnp.concatenate(
            [buf[i * peers_step + k].astype(f32) for k in range(peers_step)], axis=0
        ).astype(bf16)

    def stack(buf, dst):
        def step(i, carry):
            dst[pl.ds(pl.multiple_of(i * 16, 16), 16), :] = stacked(buf, i)
            return carry

        lax.fori_loop(0, total // 16, step, 0)

    def project(buf, weights, sums, dst, phase):
        stack(buf, xrows)
        part = jnp.dot(xrows[...], weights[...], preferred_element_type=f32)
        for p in range(n):
            sums[p] = part[p * tok : (p + 1) * tok, :]
        each_peer(lambda p: put(sums.at[p], dst.at[me], phase, p))
        keep(sums.at[me], dst.at[me], phase)

    wait_bytes(xin, recv_sem.at[0])
    wait_bytes(wq, recv_sem.at[1])
    project(xin, wq, csum, proj, 3)

    row_id = lax.broadcasted_iota(jnp.int32, (tok, LANES), 0)
    position = jnp.zeros((tok, LANES), jnp.int32)
    for s in range(tok):
        position = jnp.where(row_id == s, lengths[s], position)
    angle = position.astype(f32) * freqs[...]
    cosine, sine = jnp.cos(angle), jnp.sin(angle)
    low = lax.broadcasted_iota(jnp.int32, (tok, LANES), 1) < LANES // 2
    sine = jnp.where(low, -sine, sine)
    load_keys.wait()
    load_values.wait()
    wait_bytes(proj, recv_sem.at[3])

    def summed(buf, q):
        whole = buf[q]
        for b in range(1, blocks):
            whole = whole + buf[b * size + q]
        return whole

    projected = jnp.concatenate([summed(proj, q) for q in range(size)], axis=1)
    tiles = [projected[:, c * LANES : (c + 1) * LANES] for c in range(in_tiles)]
    turned = []
    for c in range(q_tiles + k_tiles):
        x = tiles[c]
        turned.append((x * cosine + pltpu.roll(x, LANES // 2, 1) * sine).astype(bf16).astype(f32))
    new_values = [tiles[c].astype(bf16).astype(f32) for c in range(q_tiles + k_tiles, in_tiles)]
    key_out[...] = jnp.concatenate(turned[q_tiles:], axis=1).astype(bf16)
    value_out[...] = jnp.concatenate(new_values, axis=1).astype(bf16)
    v_tiles = len(new_values) // KV_HEADS

    cache_len = keys.shape[1]
    scale = HEAD_DIM ** (-0.5)
    pairs = 2 * group
    value_dim = v_tiles * LANES
    first_map = lax.broadcasted_iota(jnp.int32, (pairs, cache_len), 0) < group
    spot = lax.broadcasted_iota(jnp.int32, (pairs, cache_len), 1)
    contract = (((1,), (1,)), ((), ()))
    out_rows = []
    for s in range(tok):
        heads = []
        for kv in range(KV_HEADS):
            q = jnp.concatenate(
                [
                    turned[(kv * group + g) * 2 + j][s : s + 1]
                    for j in range(2)
                    for g in range(group)
                ],
                axis=0,
            )
            own_key = jnp.concatenate(
                [turned[q_tiles + kv * 2 + j][s : s + 1] for j in range(2) for g in range(group)],
                axis=0,
            )
            q16 = q.astype(bf16)
            parts = [
                lax.dot_general(
                    q16,
                    keys[s, :, (kv * 2 + j) * LANES : (kv * 2 + j + 1) * LANES],
                    contract,
                    preferred_element_type=f32,
                )
                for j in range(2)
            ]
            live = spot < lengths[s]
            scores = jnp.where(live, jnp.where(first_map, parts[0], parts[1]) * scale, -jnp.inf)
            self_score = jnp.sum(q * own_key, axis=1, keepdims=True) * scale
            peak = jnp.maximum(jnp.max(scores, axis=1, keepdims=True), self_score)
            weights = jnp.exp(scores - peak)
            self_weight = jnp.exp(self_score - peak)
            totals = jnp.sum(weights, axis=1, keepdims=True) + self_weight
            map_row = lax.broadcasted_iota(jnp.int32, (pairs, 1), 0)
            factor = jnp.ones((pairs, 1), f32)
            for g in range(group):
                factor = jnp.where(map_row == group + g, lam[kv * group + g], factor)
            factor = factor / totals
            scaled = weights * factor
            self_scaled = jnp.broadcast_to(self_weight * factor, (pairs, LANES))
            combined = (scaled[:group] - scaled[group:]).astype(bf16)
            self_comb = (self_scaled[:group] - self_scaled[group:]).astype(bf16).astype(f32)
            head = jnp.dot(
                combined,
                values[s, :, kv * value_dim : (kv + 1) * value_dim],
                preferred_element_type=f32,
            )
            own_value = jnp.concatenate(
                [new_values[kv * v_tiles + v][s : s + 1] for v in range(v_tiles)], axis=1
            )
            head = head + self_comb[:, :1] * own_value
            head = head * inv_rms(head, eps_head) * head_gain[...]
            heads += [head[g : g + 1] for g in range(group)]
        out_rows.append(jnp.concatenate(heads, axis=1))
    attended = jnp.concatenate(out_rows, axis=0).astype(bf16)
    for b in range(blocks):
        abuf[b] = attended[:, b * depth : (b + 1) * depth]
    each_peer(lambda p: put(abuf.at[p // size], att.at[me], 4, p))
    keep(abuf.at[me // size], att.at[me], 4)

    wait_bytes(wo, recv_sem.at[2])
    wait_bytes(att, recv_sem.at[4])
    project(att, wo, osum, oproj, 5)
    wait_bytes(oproj, recv_sem.at[5])
    attn_proj = jnp.concatenate([summed(oproj, q) for q in range(size)], axis=1)
    after_mixer = hid[...].astype(f32) + attn_proj.astype(bf16).astype(f32)
    after_mixer = after_mixer.astype(bf16).astype(f32)
    moe_in = (after_mixer * inv_rms(after_mixer, eps_norm) * moe_gain[...]).astype(bf16)
    mbuf[...] = moe_in
    mate = me + 1 - 2 * lax.rem(me, 2)
    chips = n // 2

    def to_chip(k, carry):
        chip = lax.rem(me // 2 + chips // 2 + k, chips)
        p = chip * 2 + lax.rem(me, 2)

        @pl.when(p != me)
        def _():
            pltpu.make_async_remote_copy(
                src_ref=mbuf,
                dst_ref=gat.at[me],
                send_sem=send_sem.at[6],
                recv_sem=row_sem.at[me],
                device_id=(p,),
                device_id_type=MESH,
            ).start()

        return carry

    def send_on(k, carry):
        chip = lax.rem(me // 2 + k, chips)
        p = chip * 2 + lax.rem(me, 2)
        wait_bytes(gat.at[p], row_sem.at[p])
        pass_on(gat.at[p], p)
        return carry

    def pass_on(src, p):
        pltpu.make_async_remote_copy(
            src_ref=src,
            dst_ref=gat.at[p],
            send_sem=send_sem.at[8],
            recv_sem=recv_sem.at[6],
            device_id=(mate,),
            device_id_type=MESH,
        ).start()

    lax.fori_loop(0, chips, to_chip, 0)
    pass_on(mbuf, me)
    own_copy = load(mbuf, gat.at[me], 13)
    lax.fori_loop(1, chips, send_on, 0)
    own_copy.wait()
    wait_bytes(gat.at[pl.ds(0, chips)], recv_sem.at[6])
    stack(gat, rows16)
    load_gate.wait()
    load_up.wait()
    load_down.wait()

    def hide(block, gate_w, up_w, at):
        g = jnp.dot(block, gate_w[:, at], preferred_element_type=f32)
        u = jnp.dot(block, up_w[:, at], preferred_element_type=f32)
        return (g * jax.nn.sigmoid(g) * u).astype(bf16)

    chunk = 256
    for c in range(gate.shape[1] // chunk):
        at = slice(c * chunk, (c + 1) * chunk)
        hbuf[:, at] = hide(rows16[...], gate, up, at)
    for c in range(width // chunk):
        at = slice(c * chunk, (c + 1) * chunk)
        res[:, at] = jnp.dot(hbuf[...], down[:, at], preferred_element_type=f32)

    def split_rows(i, carry):
        block = res[pl.ds(pl.multiple_of(i * 16, 16), 16), :]
        for k in range(peers_step):
            ebuf[i * peers_step + k] = block[k * tok : (k + 1) * tok, :].astype(bf16)
        return carry

    lax.fori_loop(0, total // 16, split_rows, 0)
    each_peer(lambda p: put(ebuf.at[p], back.at[me], 7, p))
    keep(ebuf.at[me], back.at[me], 7)

    load_sgate.wait()
    load_sup.wait()
    load_sdown.wait()
    shared_hidden = jnp.concatenate(
        [
            hide(moe_in, sgate, sup, slice(c * chunk, (c + 1) * chunk))
            for c in range(sgate.shape[1] // chunk)
        ],
        axis=1,
    )
    shared_out = jnp.concatenate(
        [
            jnp.dot(
                shared_hidden,
                sdown[:, c * chunk : (c + 1) * chunk],
                preferred_element_type=f32,
            )
            for c in range(width // chunk)
        ],
        axis=1,
    )
    tokens, places = routing[...].astype(f32), route_weight[...]
    column = lax.broadcasted_iota(jnp.int32, tokens.shape, 1)
    expert_id = lax.broadcasted_iota(jnp.int32, (tokens.shape[0], n), 1).astype(f32)
    lines = []
    for s in range(tok):
        here = column == me * tok + s
        named = jnp.sum(jnp.where(here, tokens, 0.0), axis=1, keepdims=True)
        weight = jnp.sum(jnp.where(here, places, 0.0), axis=1, keepdims=True)
        chosen = jnp.where(expert_id == named, weight, 0.0)
        lines.append(jnp.sum(chosen, axis=0, keepdims=True))
    table = jnp.concatenate(lines, axis=0)
    wait_bytes(back, recv_sem.at[7])
    routed = jnp.zeros((tok, width), f32)
    for e in range(n):
        routed = routed + table[:, e : e + 1] * back[e].astype(f32)
    out_ref[...] = (after_mixer + routed + shared_out).astype(bf16)

    others, mates = pl.ds(0, n - 1), pl.ds(0, depth - rows)
    sent = (xin.at[others], wq.at[mates], wo.at[mates], proj.at[others])
    sent += (att.at[others], oproj.at[others], gat.at[pl.ds(0, n // 2 - 1)], back.at[others])
    sent += (gat.at[pl.ds(0, n // 2)],)
    for phase, ref in enumerate(sent):
        wait_bytes(ref, send_sem.at[phase])


def hand_on(*refs):
    for source, target in zip(refs[:3], refs[3:]):
        target[...] = source[...]


def on_device(
    n,
    hidden_in,
    lengths,
    key_cache,
    value_cache,
    query_w,
    key_w,
    value_w,
    out_w,
    lam_heads,
    head_gain,
    attn_gain,
    moe_gain,
    routing,
    route_weight,
    gate_w,
    up_w,
    down_w,
    shared_gate,
    shared_up,
    shared_down,
):
    tok, width = hidden_in.shape
    total = n * tok
    rows = query_w.shape[0]
    in_width = query_w.shape[1] + key_w.shape[1] + value_w.shape[1]
    size = math.gcd(in_width // LANES, width // LANES)
    depth = size * rows
    in_block, out_block = in_width // size, width // size
    half = HEAD_DIM // 2
    inverse = np.power(theta_base, -np.arange(half) / half).astype(np.float32)
    freqs = jnp.asarray(np.concatenate([inverse, inverse])[None, :])
    smem = pl.BlockSpec(memory_space=pltpu.SMEM)
    vmem = pl.BlockSpec(memory_space=pltpu.VMEM)
    hbm = pl.BlockSpec(memory_space=pl.ANY)
    like = lambda a: pltpu.VMEM(a.shape, a.dtype)
    shapes = (
        jax.ShapeDtypeStruct((tok, width), bf16),
            jax.ShapeDtypeStruct((tok, key_w.shape[1]), bf16),
            jax.ShapeDtypeStruct((tok, value_w.shape[1]), bf16),
    )
    results = pl.pallas_call(
        functools.partial(layer_kernel, n),
        out_shape=shapes,
        in_specs=[smem] * 2 + [hbm] * 13 + [vmem] * 6,
        out_specs=(vmem, vmem, vmem),
        scratch_shapes=[
            like(hidden_in),
            pltpu.VMEM((rows, in_width), bf16),
            like(out_w),
            like(key_cache),
            like(value_cache),
            pltpu.VMEM(gate_w.shape[1:], bf16),
            pltpu.VMEM(up_w.shape[1:], bf16),
            pltpu.VMEM(down_w.shape[1:], bf16),
            like(shared_gate),
            like(shared_up),
            like(shared_down),
            pltpu.VMEM((n // size, tok, depth), bf16),
            pltpu.VMEM((n, tok, depth), bf16),
            pltpu.VMEM((depth, in_block), bf16),
            pltpu.VMEM((depth, out_block), bf16),
            pltpu.VMEM((total, depth), bf16),
            pltpu.VMEM((n, tok, in_block), f32),
            pltpu.VMEM((n, tok, in_block), f32),
            pltpu.VMEM((n // size, tok, depth), bf16),
            pltpu.VMEM((n, tok, depth), bf16),
            pltpu.VMEM((n, tok, out_block), f32),
            pltpu.VMEM((n, tok, out_block), f32),
            pltpu.VMEM((tok, width), bf16),
            pltpu.VMEM((n, tok, width), bf16),
            pltpu.VMEM((total, width), bf16),
            pltpu.VMEM((total, gate_w.shape[2]), bf16),
            pltpu.VMEM((total, width), f32),
            pltpu.VMEM((n, tok, width), bf16),
            pltpu.VMEM((n, tok, width), bf16),
            pltpu.SemaphoreType.DMA((14,)),
            pltpu.SemaphoreType.DMA((9,)),
            pltpu.SemaphoreType.DMA((8,)),
            pltpu.SemaphoreType.DMA((n,)),
        ],
        compiler_params=pltpu.CompilerParams(
            collective_id=0, has_side_effects=True, vmem_limit_bytes=64000000
        ),
        name="decode_layer",
    )(
        lengths,
        lam_heads,
        hidden_in,
        key_cache,
        value_cache,
        query_w,
        key_w,
        value_w,
        out_w,
        gate_w,
        up_w,
        down_w,
        shared_gate,
        shared_up,
        shared_down,
        head_gain[None, :],
        attn_gain[None, :],
        moe_gain[None, :],
        routing.T,
        route_weight.T,
        freqs,
    )
    return pl.pallas_call(
        hand_on,
        out_shape=shapes,
        in_specs=[vmem] * 3,
        out_specs=(vmem,) * 3,
        name="hand_on",
    )(*results)


def solution(mesh):
    placed = (
        P("ep", None),
        P("ep"),
        P("ep", None, None),
        P("ep", None, None),
        P("ep", None),
        P("ep", None),
        P("ep", None),
        P("ep", None),
        P(),
        P(),
        P(),
        P(),
        P(),
        P(),
        P("ep", None, None),
        P("ep", None, None),
        P("ep", None, None),
        P(),
        P(),
        P(),
    )
    return jax.shard_map(
        functools.partial(on_device, mesh.shape["ep"]),
        mesh=mesh,
        in_specs=placed,
        out_specs=(P("ep", None), P("ep", None), P("ep", None)),
        check_vma=False,
    )
```
